32 devices in a mesh: fs: 8 (over z, y), tp: 4 (over x, core).
Axes of the slice: x: 2, y: 2, z: 4, core: 2. Of those that a mesh axis runs over, the one named last changes fastest.
Arguments:
- prompt: bfloat16 [6144, 2048], P('fs'), may hold values from -6 to 6
- routes: int32 [6144, 2], P('fs'), may hold values from 0 to 15, all different within a row; in each aligned block of 768 rows (0 to 767, 768 to 1535, ...) at most 192 rows name the same one
- affinity: float32 [6144, 2], P('fs'), may hold values from 0.05 to 1
- norm_gain: float32 [2048], P('fs'), may hold values from 0.1 to 1.9
- gate_master: float32 [16, 2048, 1024], P(None, 'fs', 'tp'), may hold values from -0.125 to 0.125
- up_master: float32 [16, 2048, 1024], P(None, 'fs', 'tp'), may hold values from -0.125 to 0.125
- down_master: float32 [16, 1024, 2048], P(None, 'fs', 'tp'), may hold values from -0.1875 to 0.1875
Outputs:
- mixed: bfloat16 [6144, 2048], P('fs', 'tp')
- gate_weights: bfloat16 [16, 2048, 1024], P('fs', None, 'tp')
- up_weights: bfloat16 [16, 2048, 1024], P('fs', None, 'tp')
- down_weights: bfloat16 [16, 1024, 2048], P('fs', None, 'tp')
The draws below stay inside these ranges and needn't reach their ends.
Inputs may be any that keep to these rules, and one draw needn't show every extreme that they name: `routes`: each row names 2 different experts. In each aligned block of 768 rows no expert is named more than 192 times, a bound that some block reaches.
All inputs are finite; a program needn't handle non-finite values.
Results may differ from the reference program's by a relative error of at most 0.0086.
Values may be sent and summed in bfloat16 or wider, within the bound.
A program may use at most 128 MiB of HBM per device.

```python
import math
import jax
import jax.numpy as jnp
import numpy as np
from jax import lax

D = 2048
FF = 1024
TOP = 2
TOK_DEV = 768
EXPERTS = 16
TOKENS = 6144
CAP = 192
N_FS = 8


def block_levels(key, extent, split, smallest, top_value):
    def one(position, parts):
        draws = jax.random.uniform(jax.random.fold_in(jax.random.fold_in(key, 6), position), (parts,), jnp.float32, smallest / len(split), top_value / len(split))
        return jnp.repeat(jnp.exp(draws), extent[position] // parts).reshape((-1,) + (1,) * (len(extent) - position - 1))

    level = one(*split[0])
    for cut in split[1:]:
        level = level * one(*cut)
    return level


def assign_block(key, own, number, rows, amount, top, most, slope):
    ranking = jax.random.permutation(key, amount)
    crowded, common = shares(amount, rows * top, most, slope, True), shares(amount, rows * top, most, slope, False)
    places = jnp.arange(amount)

    def named(lengths, turn):
        used = int((lengths > 0).sum())
        fixed = max(1, used // 4)
        moved = fixed + (places - fixed + turn * (used - fixed)) % max(1, amount - fixed)
        return jnp.zeros((amount,), jnp.int32).at[ranking[jnp.where(places < fixed, places, moved)]].set(jnp.asarray(lengths, jnp.int32))

    lengths = jnp.where(number % 4 == 0, named(crowded, number // 4), named(common, number - number // 4 - 1))
    mixed = jax.random.permutation(jax.random.fold_in(own, 3), amount)
    source_of, taker = mixed[0:amount // 2 * 2:2], mixed[1:amount // 2 * 2:2]
    margin = jnp.minimum(lengths[source_of] - 1, most - lengths[taker]) // 2
    margin = jnp.where((source_of == ranking[0]) | (taker == ranking[0]) | (lengths[taker] == 0), 0, jnp.maximum(margin, 0))
    moved = jax.random.randint(jax.random.fold_in(own, 4), (amount // 2,), 0, 1 << 20) % (margin + 1)
    lengths = lengths.at[source_of].add(-moved).at[taker].add(moved)
    labels = jnp.searchsorted(jnp.cumsum(lengths), jnp.arange(rows * top), side="right").astype(jnp.int32)
    grid = labels.reshape(top, rows).T
    grid = grid[jax.random.permutation(jax.random.fold_in(own, 1), rows)]
    turn = jax.random.randint(jax.random.fold_in(own, 2), (rows, 1), 0, top)
    return jnp.take_along_axis(grid, (jnp.arange(top)[None, :] + turn) % top, axis=1)


def shares(count, total, bound, slope, full):
    weights = [(1 << 20) // math.isqrt(rank ** slope) + 1 for rank in range(1, count + 1)]
    largest = bound if full else min(bound, max(-(-total // count), total * weights[0] // sum(weights)))
    least = 1 if total - largest >= count - 1 else 0
    counts, rest = [largest] + [least] * (count - 1), total - largest - least * (count - 1)
    while rest > 0:
        free = [i for i in range(1, count) if counts[i] < largest] or [i for i in range(1, count) if counts[i] < bound]
        whole, left = sum([weights[i] for i in free]), rest
        for i in free:
            extra = min(bound - counts[i], max(1, left * weights[i] // whole), rest)
            counts[i] = counts[i] + extra
            rest = rest - extra
    return np.array(counts)


def noise(rng, dims, width, most, pieces=(), kind=jnp.bfloat16):
    gain = block_levels(rng, dims, pieces, -0.22, 0.18) if pieces else 1.0
    drawn = jax.random.normal(rng, dims, jnp.float32) * width * gain
    return jnp.minimum(jnp.maximum(drawn, -most), most).astype(kind)


def setup_inputs(seed: int = 0) -> dict:
    arg_keys = jax.random.split(jax.random.key(seed), 8)
    prompt = noise(arg_keys[0], (TOKENS, D), 1.0, 6.0, ((0, 8),))
    routes_keys = jax.random.split(jax.random.fold_in(arg_keys[1], 1), TOKENS // TOK_DEV)
    routes_turns = jax.random.permutation(jax.random.fold_in(arg_keys[1], 3), TOKENS // TOK_DEV)
    routes = jax.vmap(lambda own, number: assign_block(jax.random.fold_in(arg_keys[1], 2), own, number, TOK_DEV, EXPERTS, TOP, CAP, 2))(routes_keys, routes_turns).reshape((TOKENS, TOP))
    affinity = jnp.clip(0.05 + 0.95 * jax.random.uniform(arg_keys[2], (TOKENS, TOP), jnp.float32) ** block_levels(arg_keys[2], (TOKENS, TOP), ((0, 8),), -0.2, 0.2), 0.05, 1.0)
    norm_gain = jnp.clip(1.0 + 0.18 * jax.random.normal(arg_keys[3], (D,), jnp.float32), 0.1, 1.9)
    gate_master = noise(arg_keys[4], (EXPERTS, D, FF), D ** -0.5, 0.125, ((1, 8), (2, 4)), jnp.float32)
    up_master = noise(arg_keys[5], (EXPERTS, D, FF), D ** -0.5, 0.125, ((1, 8), (2, 4)), jnp.float32)
    down_master = noise(arg_keys[6], (EXPERTS, FF, D), FF ** -0.5, 0.1875, ((1, 8), (2, 4)), jnp.float32)
    return {"prompt": prompt, "routes": routes, "affinity": affinity, "norm_gain": norm_gain, "gate_master": gate_master, "up_master": up_master, "down_master": down_master}


norm_eps = 1e-06

def one_expert(operands):
    slot_rows, gate_weight, up_weight, down_weight = operands
    gate_pre = jnp.dot(slot_rows, gate_weight, preferred_element_type=jnp.float32)
    up_pre = jnp.dot(slot_rows, up_weight, preferred_element_type=jnp.float32)
    hidden = (jax.nn.silu(gate_pre) * up_pre).astype(jnp.bfloat16)
    return jnp.dot(hidden, down_weight, preferred_element_type=jnp.float32).astype(jnp.bfloat16)

def reference(prompt, routes, affinity, norm_gain, gate_master, up_master, down_master):
    gain_rows = norm_gain[None, :, None]
    gate_weights = (gate_master * gain_rows).astype(jnp.bfloat16)
    up_weights = (up_master * gain_rows).astype(jnp.bfloat16)
    down_weights = down_master.astype(jnp.bfloat16)
    values = prompt.astype(jnp.float32)
    normed = (values * lax.rsqrt(lax.optimization_barrier(jnp.mean(values * values, axis=-1, keepdims=True)) + norm_eps)).astype(jnp.bfloat16)
    flat_ids = routes.reshape(N_FS, TOK_DEV * TOP)
    onehot = (flat_ids[:, :, None] == jnp.arange(EXPERTS, dtype=jnp.int32)[None, None, :]).astype(jnp.int32)
    slot_rank = lax.optimization_barrier(jnp.sum(jnp.cumsum(onehot, axis=1) * onehot, axis=2)) - 1
    column = (jnp.arange(N_FS, dtype=jnp.int32)[:, None] * CAP + slot_rank).reshape(-1).astype(jnp.int32)
    expert_of = flat_ids.reshape(-1).astype(jnp.int32)
    token_of = (jnp.arange(TOKENS * TOP, dtype=jnp.int32) // TOP).astype(jnp.int32)
    buffer = jnp.zeros((EXPERTS, N_FS * CAP, D), jnp.bfloat16).at[expert_of, column].set(normed[token_of])
    outputs = lax.map(one_expert, (buffer, gate_weights, up_weights, down_weights))
    picked = outputs[expert_of, column].reshape(TOKENS, TOP, D).astype(jnp.float32)
    share = affinity / lax.optimization_barrier(jnp.sum(affinity, axis=1, keepdims=True))
    mixed = lax.optimization_barrier(jnp.sum(share[:, :, None] * picked, axis=1)).astype(jnp.bfloat16)
    return (mixed, gate_weights, up_weights, down_weights)
```

```python
import functools

import jax
import jax.numpy as jnp
from jax import lax
from jax.experimental import pallas as pl
from jax.experimental.pallas import tpu as pltpu
from jax.sharding import PartitionSpec as P

norm_eps = 1e-06
MESH = pl.DeviceIdType.MESH


def remote(src, dst, send_sem, recv_sem, where):
    return pltpu.make_async_remote_copy(
        src_ref=src,
        dst_ref=dst,
        send_sem=send_sem,
        recv_sem=recv_sem,
        device_id=where,
        device_id_type=MESH,
    )


def loop(first, last, body):
    def step(i, carry):
        body(i)
        return carry

    lax.fori_loop(first, last, step, 0)


class Spread:
    def __init__(self, tp, whole, rows_of, width, sems):
        self.chips = tp // 2
        self.me = lax.axis_index("tp")
        self.chip, self.core = self.me // 2, self.me % 2
        self.whole, self.rows_of, self.width = whole, rows_of, width
        self.first_send, self.first_recv, self.relay_send, self.relay_recv = sems

    def greet(self, barrier):
        for hop in range(self.chips):
            pl.semaphore_signal(barrier, inc=1, device_id={"tp": self.target(hop)}, device_id_type=MESH)
        return self.chips

    def target(self, hop):
        if hop == 0:
            return self.chip * 2 + 1 - self.core
        return lax.rem(self.chip + hop, self.chips) * 2 + self.core

    def block(self, chunk, owner):
        return self.whole.at[:, self.rows_of(chunk), pl.ds(pl.multiple_of(owner * self.width, self.width), self.width)]

    def first(self, chunk, hop):
        mine = self.block(chunk, self.me)
        return remote(mine, mine, self.first_send.at[chunk, hop], self.first_recv.at[chunk, hop], {"tp": self.target(hop)})

    def relay(self, chunk, hop):
        owner = lax.rem(self.chip - hop + self.chips, self.chips) * 2 + self.core
        taken = self.block(chunk, owner)
        return remote(taken, taken, self.relay_send.at[chunk, hop], self.relay_recv.at[chunk, hop], {"tp": self.target(0)})

    def start(self, chunk):
        for hop in [*range(1, self.chips), 0]:
            self.first(chunk, hop).start()

    def hand_on(self, chunk):
        for hop in range(1, self.chips):
            self.first(chunk, hop).wait_recv()
            self.relay(chunk, hop).start()

    def finish(self, chunk):
        self.first(chunk, 0).wait_recv()
        for hop in range(self.chips):
            self.first(chunk, hop).wait_send()
        for hop in range(1, self.chips):
            self.relay(chunk, hop).wait()


def spread_sems(n, tp):
    return [pltpu.SemaphoreType.DMA((n, tp // 2))] * 4


def peer(step, n):
    return lax.rem(lax.axis_index("fs") + step, n)


def source(step, n):
    return lax.rem(lax.axis_index("fs") - step + n, n)


class Weights:
    def __init__(self, n, master, gain, out, raw, send, sems):
        self.n, self.master, self.gain, self.out, self.raw, self.send = n, master, gain, out, raw, send
        self.load_sem, self.send_sem, self.recv_sem = sems
        self.keep, self.rows = master.shape[0] // n, master.shape[1]

    def load(self, step):
        return pltpu.make_async_copy(
            self.master.at[pl.ds(peer(step, self.n) * self.keep, self.keep)], self.raw.at[step], self.load_sem.at[step]
        )

    def place(self):
        me = lax.axis_index("fs")
        return self.out.at[:, pl.ds(pl.multiple_of(me * self.rows, self.rows), self.rows), :]

    def copy(self, step):
        return remote(
            self.send.at[step], self.place(), self.send_sem.at[step], self.recv_sem.at[step], {"fs": peer(step, self.n)}
        )

    def own(self):
        return pltpu.make_async_copy(self.send.at[0], self.place(), self.send_sem.at[0])

    def load_all(self):
        for step in [*range(1, self.n), 0]:
            self.load(step).start()

    def cast(self, step):
        self.load(step).wait()
        block = self.raw[step]
        if self.gain is not None:
            block = block * self.gain[...][None]
        self.send[step] = block.astype(jnp.bfloat16)

    def send_all(self):
        self.cast(1)

        def body(step):
            self.cast(step)
            self.copy(step - 1).start()

        loop(2, self.n, body)
        self.cast(0)
        self.copy(self.n - 1).start()
        self.own().start()

    def finish(self):
        self.own().wait()
        loop(1, self.n, lambda step: self.copy(step).wait())


def greet_all(n, spread):
    barrier = pltpu.get_barrier_semaphore()
    for step in range(1, n):
        pl.semaphore_signal(barrier, inc=1, device_id={"fs": peer(step, n)}, device_id_type=MESH)
    amount = spread.greet(barrier)
    pl.semaphore_wait(barrier, n - 1 + amount)


def dispatch_kernel(n, tp, gain, outbox, gate, up, gate_out, up_out, gathered, *refs):
    gate_raw, up_raw, gate_send, up_send, weight_sems, token_send, token_recv = refs[:7]
    keep, (_, capacity, width) = outbox.shape[0] // n, outbox.shape
    me = lax.axis_index("fs")
    parts = [
        Weights(n, gate, gain, gate_out, gate_raw, gate_send, [weight_sems.at[0, i] for i in range(3)]),
        Weights(n, up, gain, up_out, up_raw, up_send, [weight_sems.at[1, i] for i in range(3)]),
    ]

    def rows_of(chunk):
        return pl.ds(pl.multiple_of(source(chunk, n) * capacity, capacity), capacity)

    spread = Spread(tp, gathered, rows_of, width, refs[7:11])
    column = pl.ds(pl.multiple_of(lax.axis_index("tp") * width, width), width)

    def token(step):
        return remote(
            outbox.at[pl.ds(peer(step, n) * keep, keep)],
            gathered.at[:, pl.ds(pl.multiple_of(me * capacity, capacity), capacity), column],
            token_send.at[step],
            token_recv.at[step],
            {"fs": peer(step, n)},
        )

    own = pltpu.make_async_copy(
        outbox.at[pl.ds(me * keep, keep)], spread.block(0, lax.axis_index("tp")), token_send.at[0]
    )
    own.start()
    for part in parts:
        part.load_all()
    greet_all(n, spread)
    loop(1, n, lambda step: token(step).start())
    own.wait()
    spread.start(0)
    for part in parts:
        part.send_all()

    def body(step):
        token(step).wait_recv()
        spread.start(step)
        spread.hand_on(step - 1)

    loop(1, n, body)
    spread.hand_on(n - 1)
    loop(1, n, lambda step: token(step).wait_send())
    loop(0, n, spread.finish)
    for part in parts:
        part.finish()


def weight_shapes(master, n):
    experts, rows, columns = master.shape
    keep = experts // n
    return (
        jax.ShapeDtypeStruct((keep, rows * n, columns), jnp.bfloat16),
        pltpu.VMEM((n, keep, rows, columns), jnp.float32),
        pltpu.VMEM((n, keep, rows, columns), jnp.bfloat16),
    )


def dispatch(gain, outbox, gate, up):
    n, tp = lax.axis_size("fs"), lax.axis_size("tp")
    experts, capacity, width = outbox.shape
    gate_out, gate_raw, gate_send = weight_shapes(gate, n)
    up_out, up_raw, up_send = weight_shapes(up, n)
    inside, anywhere = pl.BlockSpec(memory_space=pltpu.VMEM), pl.BlockSpec(memory_space=pl.ANY)
    return pl.pallas_call(
        functools.partial(dispatch_kernel, n, tp),
        out_shape=[
            gate_out,
            up_out,
            jax.ShapeDtypeStruct((experts // n, n * capacity, width * tp), jnp.bfloat16),
        ],
        in_specs=[inside, inside, anywhere, anywhere],
        out_specs=[anywhere] * 3,
        scratch_shapes=[gate_raw, up_raw, gate_send, up_send]
        + [pltpu.SemaphoreType.DMA((2, 3, n))]
        + [pltpu.SemaphoreType.DMA((n,))] * 2
        + spread_sems(n, tp),
        compiler_params=pltpu.CompilerParams(
            collective_id=0, has_side_effects=True, vmem_limit_bytes=48 * 2**20
        ),
        name="dispatch",
    )(gain[:, None], outbox, gate, up)


def combine_kernel(n, tp, hidden, down, down_out, returned, *refs):
    raw, send, held, whole, out, weight_sems, back_send, back_recv, local_sem = refs[:9]
    keep, rows, width = hidden.shape
    capacity = rows // n
    me = lax.axis_index("fs")
    part = Weights(n, down, None, held, raw, send, [weight_sems.at[i] for i in range(3)])

    def rows_of(chunk):
        return pl.ds(pl.multiple_of(peer(chunk, n) * capacity, capacity), capacity)

    spread = Spread(tp, whole, rows_of, width, refs[9:13])

    def own(chunk):
        return pltpu.make_async_copy(
            hidden.at[:, rows_of(chunk), :], spread.block(chunk, lax.axis_index("tp")), local_sem.at[chunk]
        )

    part.load_all()
    loop(0, n, lambda chunk: own(chunk).start())
    greet_all(n, spread)

    def begin(chunk):
        own(chunk).wait()
        spread.start(chunk)

    loop(0, n, begin)
    part.send_all()
    loop(0, n, spread.hand_on)
    loop(0, n, spread.finish)
    part.finish()
    keeping = pltpu.make_async_copy(held, down_out, local_sem.at[0])
    keeping.start()

    def back(step):
        return remote(
            out.at[step], returned.at[me], back_send.at[step], back_recv.at[step], {"fs": peer(step, n)}
        )

    def multiply(step):
        for e in range(keep):
            out[step, e] = jnp.dot(
                whole[e, rows_of(step), :], held[e], preferred_element_type=jnp.float32
            ).astype(jnp.bfloat16)

    multiply(1)

    def body(step):
        multiply(step)
        back(step - 1).start()

    loop(2, n, body)
    multiply(0)
    back(n - 1).start()
    mine = pltpu.make_async_copy(out.at[0], returned.at[me], back_send.at[0])
    mine.start()
    keeping.wait()
    mine.wait()
    loop(1, n, lambda step: back(step).wait())


def combine(hidden, down):
    n, tp = lax.axis_size("fs"), lax.axis_size("tp")
    keep, rows, width = hidden.shape
    down_out, raw, send = weight_shapes(down, n)
    columns = down.shape[2]
    block = (n, keep, rows // n, columns)
    inside, anywhere = pl.BlockSpec(memory_space=pltpu.VMEM), pl.BlockSpec(memory_space=pl.ANY)
    return pl.pallas_call(
        functools.partial(combine_kernel, n, tp),
        out_shape=[down_out, jax.ShapeDtypeStruct(block, jnp.bfloat16)],
        in_specs=[inside, anywhere],
        out_specs=[anywhere] * 2,
        scratch_shapes=[
            raw,
            send,
            pltpu.VMEM(down_out.shape, jnp.bfloat16),
            pltpu.VMEM((keep, rows, width * tp), jnp.bfloat16),
            pltpu.VMEM(block, jnp.bfloat16),
            pltpu.SemaphoreType.DMA((3, n)),
            pltpu.SemaphoreType.DMA((n,)),
            pltpu.SemaphoreType.DMA((n,)),
            pltpu.SemaphoreType.DMA((n,)),
        ]
        + spread_sems(n, tp),
        compiler_params=pltpu.CompilerParams(
            collective_id=1, has_side_effects=True, vmem_limit_bytes=48 * 2**20
        ),
        name="combine",
    )(hidden, down)


def per_device(prompt, routes, affinity, norm_gain, gate_master, up_master, down_master):
    tp_count = lax.axis_size("tp")
    experts = gate_master.shape[0]
    token_count, model_width = prompt.shape
    top_count = routes.shape[1]
    capacity = 2 * token_count * top_count // experts

    values = prompt.astype(jnp.float32)
    scale = lax.rsqrt(jnp.mean(values * values, axis=-1, keepdims=True) + norm_eps)
    column_width = model_width // tp_count
    columns = lax.dynamic_slice_in_dim(
        prompt, lax.axis_index("tp") * column_width, column_width, 1
    )
    normed = (columns.astype(jnp.float32) * scale).astype(jnp.bfloat16)

    names = jnp.arange(experts, dtype=jnp.int32)
    hits = (routes.T[:, None, :] == names[None, :, None]).astype(jnp.float32)
    named = jnp.sum(hits, axis=0)
    position = jnp.arange(token_count, dtype=jnp.int32)
    earlier = (position[:, None] < position[None, :]).astype(jnp.bfloat16)
    rank = jnp.dot(named.astype(jnp.bfloat16), earlier, preferred_element_type=jnp.float32)
    slot = jnp.where(named > 0, rank, -1.0).astype(jnp.int32)
    share = (affinity / jnp.sum(affinity, axis=1, keepdims=True)).T
    weight = jnp.sum(hits * share[:, None, :], axis=0)

    places = jnp.arange(capacity, dtype=jnp.int32)
    pick = (slot[:, None, :] == places[None, :, None]).astype(jnp.bfloat16)
    outbox = jnp.einsum(
        "ert,td->erd", pick, normed, preferred_element_type=jnp.float32
    ).astype(jnp.bfloat16)

    gate_new, up_new, gathered = dispatch(norm_gain, outbox, gate_master, up_master)
    gate_pre = jnp.einsum("erd,edf->erf", gathered, gate_new, preferred_element_type=jnp.float32)
    up_pre = jnp.einsum("erd,edf->erf", gathered, up_new, preferred_element_type=jnp.float32)
    hidden = (jax.nn.silu(gate_pre) * up_pre).astype(jnp.bfloat16)
    down_new, returned = combine(hidden, down_master)

    spread = jnp.where(
        slot[:, None, :] == places[None, :, None], weight[:, None, :], 0
    ).astype(jnp.bfloat16)
    mixed = lax.dot_general(
        spread.reshape(experts * capacity, token_count),
        returned.reshape(experts * capacity, -1),
        (((0,), (0,)), ((), ())),
        preferred_element_type=jnp.float32,
    ).astype(jnp.bfloat16)
    return (mixed, gate_new, up_new, down_new)


def solution(mesh):
    in_specs = (
        P("fs", None),
        P("fs", None),
        P("fs", None),
        P("fs"),
        P(None, "fs", "tp"),
        P(None, "fs", "tp"),
        P(None, "fs", "tp"),
    )
    out_specs = (P("fs", "tp"), P("fs", None, "tp"), P("fs", None, "tp"), P("fs", None, "tp"))
    return jax.shard_map(
        per_device, mesh=mesh, in_specs=in_specs, out_specs=out_specs, check_vma=False
    )
```

```python
import functools

import jax
import jax.numpy as jnp
from jax import lax
from jax.experimental import pallas as pl
from jax.experimental.pallas import tpu as pltpu
from jax.sharding import PartitionSpec as P

norm_eps = 1e-06
MESH = pl.DeviceIdType.MESH


def remote(src, dst, send_sem, recv_sem, where):
    return pltpu.make_async_remote_copy(
        src_ref=src,
        dst_ref=dst,
        send_sem=send_sem,
        recv_sem=recv_sem,
        device_id=where,
        device_id_type=MESH,
    )


def loop(first, last, body):
    def step(i, carry):
        body(i)
        return carry

    lax.fori_loop(first, last, step, 0)


class Spread:
    def __init__(self, tp, whole, rows_of, width, sems):
        self.chips = tp // 2
        self.me = lax.axis_index("tp")
        self.chip, self.core = self.me // 2, self.me % 2
        self.whole, self.rows_of, self.width = whole, rows_of, width
        self.first_send, self.first_recv, self.relay_send, self.relay_recv = sems

    def greet(self, barrier):
        for hop in range(self.chips):
            pl.semaphore_signal(barrier, inc=1, device_id={"tp": self.target(hop)}, device_id_type=MESH)
        return self.chips

    def target(self, hop):
        if hop == 0:
            return self.chip * 2 + 1 - self.core
        return lax.rem(self.chip + hop, self.chips) * 2 + self.core

    def block(self, chunk, owner):
        return self.whole.at[:, self.rows_of(chunk), pl.ds(pl.multiple_of(owner * self.width, self.width), self.width)]

    def first(self, chunk, hop):
        mine = self.block(chunk, self.me)
        return remote(mine, mine, self.first_send.at[chunk, hop], self.first_recv.at[chunk, hop], {"tp": self.target(hop)})

    def relay(self, chunk, hop):
        owner = lax.rem(self.chip - hop + self.chips, self.chips) * 2 + self.core
        taken = self.block(chunk, owner)
        return remote(taken, taken, self.relay_send.at[chunk, hop], self.relay_recv.at[chunk, hop], {"tp": self.target(0)})

    def start(self, chunk):
        for hop in [*range(1, self.chips), 0]:
            self.first(chunk, hop).start()

    def hand_on(self, chunk):
        for hop in range(1, self.chips):
            self.first(chunk, hop).wait_recv()
            self.relay(chunk, hop).start()

    def finish(self, chunk):
        self.first(chunk, 0).wait_recv()
        for hop in range(self.chips):
            self.first(chunk, hop).wait_send()
        for hop in range(1, self.chips):
            self.relay(chunk, hop).wait()


def spread_sems(n, tp):
    return [pltpu.SemaphoreType.DMA((n, tp // 2))] * 4


def peer(step, n):
    return lax.rem(lax.axis_index("fs") + step, n)


def source(step, n):
    return lax.rem(lax.axis_index("fs") - step + n, n)


class Weights:
    def __init__(self, n, master, gain, out, raw, send, sems):
        self.n, self.master, self.gain, self.out, self.raw, self.send = n, master, gain, out, raw, send
        self.load_sem, self.send_sem, self.recv_sem = sems
        self.keep, self.rows = master.shape[0] // n, master.shape[1]

    def load(self, step):
        return pltpu.make_async_copy(
            self.master.at[pl.ds(peer(step, self.n) * self.keep, self.keep)], self.raw.at[step], self.load_sem.at[step]
        )

    def place(self):
        me = lax.axis_index("fs")
        return self.out.at[:, pl.ds(pl.multiple_of(me * self.rows, self.rows), self.rows), :]

    def copy(self, step):
        return remote(
            self.send.at[step], self.place(), self.send_sem.at[step], self.recv_sem.at[step], {"fs": peer(step, self.n)}
        )

    def own(self):
        return pltpu.make_async_copy(self.send.at[0], self.place(), self.send_sem.at[0])

    def load_all(self):
        for step in [*range(1, self.n), 0]:
            self.load(step).start()

    def cast(self, step):
        self.load(step).wait()
        block = self.raw[step]
        if self.gain is not None:
            block = block * self.gain[...][None]
        self.send[step] = block.astype(jnp.bfloat16)

    def send_all(self):
        self.cast(1)

        def body(step):
            self.cast(step)
            self.copy(step - 1).start()

        loop(2, self.n, body)
        self.cast(0)
        self.copy(self.n - 1).start()
        self.own().start()

    def finish(self):
        self.own().wait()
        loop(1, self.n, lambda step: self.copy(step).wait())


def greet_all(n, spread):
    barrier = pltpu.get_barrier_semaphore()
    for step in range(1, n):
        pl.semaphore_signal(barrier, inc=1, device_id={"fs": peer(step, n)}, device_id_type=MESH)
    amount = spread.greet(barrier)
    pl.semaphore_wait(barrier, n - 1 + amount)


def dispatch_kernel(n, tp, gain, outbox, gate, up, gate_out, up_out, gathered, *refs):
    gate_raw, up_raw, gate_send, up_send, weight_sems, token_send, token_recv = refs[:7]
    keep, (_, capacity, width) = outbox.shape[0] // n, outbox.shape
    me = lax.axis_index("fs")
    parts = [
        Weights(n, gate, gain, gate_out, gate_raw, gate_send, [weight_sems.at[0, i] for i in range(3)]),
        Weights(n, up, gain, up_out, up_raw, up_send, [weight_sems.at[1, i] for i in range(3)]),
    ]

    def rows_of(chunk):
        return pl.ds(pl.multiple_of(source(chunk, n) * capacity, capacity), capacity)

    spread = Spread(tp, gathered, rows_of, width, refs[7:11])
    column = pl.ds(pl.multiple_of(lax.axis_index("tp") * width, width), width)

    def token(step):
        return remote(
            outbox.at[pl.ds(peer(step, n) * keep, keep)],
            gathered.at[:, pl.ds(pl.multiple_of(me * capacity, capacity), capacity), column],
            token_send.at[step],
            token_recv.at[step],
            {"fs": peer(step, n)},
        )

    own = pltpu.make_async_copy(
        outbox.at[pl.ds(me * keep, keep)], spread.block(0, lax.axis_index("tp")), token_send.at[0]
    )
    own.start()
    for part in parts:
        part.load_all()
    greet_all(n, spread)
    loop(1, n, lambda step: token(step).start())
    own.wait()
    spread.start(0)
    for part in parts:
        part.send_all()

    def body(step):
        token(step).wait_recv()
        spread.start(step)
        spread.hand_on(step - 1)

    loop(1, n, body)
    spread.hand_on(n - 1)
    loop(1, n, lambda step: token(step).wait_send())
    loop(0, n, spread.finish)
    for part in parts:
        part.finish()


def weight_shapes(master, n):
    experts, rows, columns = master.shape
    keep = experts // n
    return (
        jax.ShapeDtypeStruct((keep, rows * n, columns), jnp.bfloat16),
        pltpu.VMEM((n, keep, rows, columns), jnp.float32),
        pltpu.VMEM((n, keep, rows, columns), jnp.bfloat16),
    )


def dispatch(gain, outbox, gate, up):
    n, tp = lax.axis_size("fs"), lax.axis_size("tp")
    experts, capacity, width = outbox.shape
    gate_out, gate_raw, gate_send = weight_shapes(gate, n)
    up_out, up_raw, up_send = weight_shapes(up, n)
    inside, anywhere = pl.BlockSpec(memory_space=pltpu.VMEM), pl.BlockSpec(memory_space=pl.ANY)
    return pl.pallas_call(
        functools.partial(dispatch_kernel, n, tp),
        out_shape=[
            gate_out,
            up_out,
            jax.ShapeDtypeStruct((experts // n, n * capacity, width * tp), jnp.bfloat16),
        ],
        in_specs=[inside, inside, anywhere, anywhere],
        out_specs=[anywhere] * 3,
        scratch_shapes=[gate_raw, up_raw, gate_send, up_send]
        + [pltpu.SemaphoreType.DMA((2, 3, n))]
        + [pltpu.SemaphoreType.DMA((n,))] * 2
        + spread_sems(n, tp),
        compiler_params=pltpu.CompilerParams(
            collective_id=0, has_side_effects=True, vmem_limit_bytes=48 * 2**20
        ),
        name="dispatch",
    )(gain[:, None], outbox, gate, up)


def combine_kernel(n, tp, gathered, gate, up, down, down_out, returned, *refs):
    raw, send, held, whole, out, taken, gate_in, up_in = refs[:8]
    weight_sems, back_send, back_recv, local_sem, in_sem = refs[8:13]
    keep, rows, _ = gathered.shape
    width = gate.shape[2]
    capacity = rows // n
    me = lax.axis_index("fs")
    part = Weights(n, down, None, held, raw, send, [weight_sems.at[i] for i in range(3)])

    def rows_of(chunk):
        return pl.ds(pl.multiple_of(peer(chunk, n) * capacity, capacity), capacity)

    spread = Spread(tp, whole, rows_of, width, refs[13:17])
    column = pl.ds(pl.multiple_of(lax.axis_index("tp") * width, width), width)

    def take(chunk):
        return pltpu.make_async_copy(
            gathered.at[:, rows_of(chunk), :], taken.at[:, rows_of(chunk), :], in_sem.at[chunk]
        )

    weights = [
        pltpu.make_async_copy(gate, gate_in, in_sem.at[n]),
        pltpu.make_async_copy(up, up_in, in_sem.at[n + 1]),
    ]

    part.load_all()
    for weight in weights:
        weight.start()
    loop(0, n, lambda chunk: take(chunk).start())
    greet_all(n, spread)
    part.send_all()
    for weight in weights:
        weight.wait()

    def produce(chunk):
        take(chunk).wait()
        for e in range(keep):
            block = taken[e, rows_of(chunk), :]
            gate_pre = jnp.dot(block, gate_in[e], preferred_element_type=jnp.float32)
            up_pre = jnp.dot(block, up_in[e], preferred_element_type=jnp.float32)
            hidden = gate_pre / (1.0 + jnp.exp(-gate_pre)) * up_pre
            whole[e, rows_of(chunk), column] = hidden.astype(jnp.bfloat16)

    def advance(chunk):
        produce(chunk)
        spread.start(chunk - 1)
        spread.hand_on(chunk - 2)

    produce(0)
    produce(1)
    spread.start(0)
    loop(2, n, advance)
    spread.start(n - 1)
    loop(n - 2, n, spread.hand_on)
    loop(0, n, spread.finish)
    part.finish()
    keeping = pltpu.make_async_copy(held, down_out, local_sem.at[0])
    keeping.start()

    def back(step):
        return remote(
            out.at[step], returned.at[me], back_send.at[step], back_recv.at[step], {"fs": peer(step, n)}
        )

    def multiply(step):
        for e in range(keep):
            out[step, e] = jnp.dot(
                whole[e, rows_of(step), :], held[e], preferred_element_type=jnp.float32
            ).astype(jnp.bfloat16)

    multiply(1)

    def body(step):
        multiply(step)
        back(step - 1).start()

    loop(2, n, body)
    multiply(0)
    back(n - 1).start()
    mine = pltpu.make_async_copy(out.at[0], returned.at[me], back_send.at[0])
    mine.start()
    keeping.wait()
    mine.wait()
    loop(1, n, lambda step: back(step).wait())


def combine(gathered, gate, up, down):
    n, tp = lax.axis_size("fs"), lax.axis_size("tp")
    (keep, rows, _), width = gathered.shape, gate.shape[2]
    down_out, raw, send = weight_shapes(down, n)
    columns = down.shape[2]
    block = (n, keep, rows // n, columns)
    anywhere = pl.BlockSpec(memory_space=pl.ANY)
    return pl.pallas_call(
        functools.partial(combine_kernel, n, tp),
        out_shape=[down_out, jax.ShapeDtypeStruct(block, jnp.bfloat16)],
        in_specs=[anywhere] * 4,
        out_specs=[anywhere] * 2,
        scratch_shapes=[
            raw,
            send,
            pltpu.VMEM(down_out.shape, jnp.bfloat16),
            pltpu.VMEM((keep, rows, width * tp), jnp.bfloat16),
            pltpu.VMEM(block, jnp.bfloat16),
            pltpu.VMEM(gathered.shape, jnp.bfloat16),
            pltpu.VMEM(gate.shape, jnp.bfloat16),
            pltpu.VMEM(up.shape, jnp.bfloat16),
            pltpu.SemaphoreType.DMA((3, n)),
            pltpu.SemaphoreType.DMA((n,)),
            pltpu.SemaphoreType.DMA((n,)),
            pltpu.SemaphoreType.DMA((n,)),
            pltpu.SemaphoreType.DMA((n + 2,)),
        ]
        + spread_sems(n, tp),
        compiler_params=pltpu.CompilerParams(
            collective_id=1, has_side_effects=True, vmem_limit_bytes=48 * 2**20
        ),
        name="combine",
    )(gathered, gate, up, down)


def per_device(prompt, routes, affinity, norm_gain, gate_master, up_master, down_master):
    tp_count = lax.axis_size("tp")
    experts = gate_master.shape[0]
    token_count, model_width = prompt.shape
    top_count = routes.shape[1]
    capacity = 2 * token_count * top_count // experts

    values = prompt.astype(jnp.float32)
    scale = lax.rsqrt(jnp.mean(values * values, axis=-1, keepdims=True) + norm_eps)
    column_width = model_width // tp_count
    columns = lax.dynamic_slice_in_dim(
        prompt, lax.axis_index("tp") * column_width, column_width, 1
    )
    normed = (columns.astype(jnp.float32) * scale).astype(jnp.bfloat16)

    names = jnp.arange(experts, dtype=jnp.int32)
    hits = (routes.T[:, None, :] == names[None, :, None]).astype(jnp.float32)
    named = jnp.sum(hits, axis=0)
    position = jnp.arange(token_count, dtype=jnp.int32)
    earlier = (position[:, None] < position[None, :]).astype(jnp.bfloat16)
    rank = jnp.dot(named.astype(jnp.bfloat16), earlier, preferred_element_type=jnp.float32)
    slot = jnp.where(named > 0, rank, -1.0).astype(jnp.int32)
    share = (affinity / jnp.sum(affinity, axis=1, keepdims=True)).T
    weight = jnp.sum(hits * share[:, None, :], axis=0)

    places = jnp.arange(capacity, dtype=jnp.int32)
    pick = (slot[:, None, :] == places[None, :, None]).astype(jnp.bfloat16)
    outbox = jnp.einsum(
        "ert,td->erd", pick, normed, preferred_element_type=jnp.float32
    ).astype(jnp.bfloat16)

    gate_new, up_new, gathered = dispatch(norm_gain, outbox, gate_master, up_master)
    down_new, returned = combine(gathered, gate_new, up_new, down_master)

    spread = jnp.where(
        slot[:, None, :] == places[None, :, None], weight[:, None, :], 0
    ).astype(jnp.bfloat16)
    mixed = lax.dot_general(
        spread.reshape(experts * capacity, token_count),
        returned.reshape(experts * capacity, -1),
        (((0,), (0,)), ((), ())),
        preferred_element_type=jnp.float32,
    ).astype(jnp.bfloat16)
    return (mixed, gate_new, up_new, down_new)


def solution(mesh):
    in_specs = (
        P("fs", None),
        P("fs", None),
        P("fs", None),
        P("fs"),
        P(None, "fs", "tp"),
        P(None, "fs", "tp"),
        P(None, "fs", "tp"),
    )
    out_specs = (P("fs", "tp"), P("fs", None, "tp"), P("fs", None, "tp"), P("fs", None, "tp"))
    return jax.shard_map(
        per_device, mesh=mesh, in_specs=in_specs, out_specs=out_specs, check_vma=False
    )
```
